32 devices in a mesh: sp: 8 (over z, x), tp: 4 (over y, core).
Axes of the slice: x: 2, y: 2, z: 4, core: 2. Of those that a mesh axis runs over, the one named last changes fastest.
Arguments:
- hidden_in: bfloat16 [2, 12288, 2048], P(None, ('sp', 'tp')), may hold values from -6 to 6
- w_value: bfloat16 [2048, 2048], P(None, 'tp'), may hold values from -0.125 to 0.125
- w_key: bfloat16 [2048, 2048], P(None, 'tp'), may hold values from -0.125 to 0.125
- w_step: bfloat16 [2048, 32], replicated, may hold values from -0.125 to 0.125
- conv_value: bfloat16 [4, 2048], P(None, 'tp'), may hold values from -3 to 3
- conv_key: bfloat16 [4, 2048], P(None, 'tp'), may hold values from -3 to 3
- step_bias: float32 [32], P('tp'), may hold values from -3 to -1
- decay_rate: float32 [32], P('tp'), may hold values from 8.138021e-06 to 0.25
- decay_jump: float32 [2, 12288, 32], P(None, 'sp', 'tp'), may hold values from -0.75 to 0
- new_value: bfloat16 [2, 2048], P(None, 'tp'), may hold values from -60 to 60
- new_key: bfloat16 [2, 2048], P(None, 'tp'), may hold values from -6 to 6
- new_query: bfloat16 [2, 2048], P(None, 'tp'), may hold values from -6 to 6
- new_gate: bfloat16 [2, 2048], P(None, 'tp'), may hold values from -6 to 6
- new_step: float32 [2, 32], P(None, 'tp'), may hold values from -6 to 6
- read_gain: bfloat16 [2048], P('tp'), may hold values from 0.099609375 to 1.8984375
Outputs:
- prompt_state: bfloat16 [2, 32, 64, 128], P(None, 'tp', 'sp')
- read_out: bfloat16 [2, 32, 64], P(None, 'tp', 'sp')
The draws below stay inside these ranges and needn't reach their ends.
All inputs are finite; a program needn't handle non-finite values.
Results may differ from the reference program's by a relative error of at most 0.006.
Values may be sent and summed in bfloat16 or wider, within the bound.
A program may use at most 64 MiB of HBM per device.

```python
import jax
import jax.numpy as jnp
from jax import lax

D = 2048
HEADS = 32
HEAD_DIM = 64
STATE = 128
GROUPS = 16
KERNEL = 4
PROMPT_COUNT = 2
SEG = 1536
PROMPT_LENGTH = 12288


def draw_decay_rate(key, part):
    uniform_draw = jax.random.uniform(key, (HEADS,), jnp.float32)
    bottom = 0.1 / PROMPT_LENGTH
    summit = 0.25
    return jnp.exp(jnp.log(bottom) + uniform_draw * (jnp.log(summit) - jnp.log(bottom)))


def draw_decay_jump(key, part):
    drain_key, noise_key, location_random_key, magnitude_random_key = jax.random.split(key, 4)
    blocks = PROMPT_LENGTH // SEG
    uniform_draw = jax.random.uniform(drain_key, (PROMPT_COUNT, blocks, 1, HEADS), jnp.float32)
    bottom_log = jnp.log(0.1)
    summit_log = jnp.log(1.0)
    leakage_rate = jnp.exp(bottom_log + uniform_draw * (summit_log - bottom_log)) / PROMPT_LENGTH
    roughness = jax.random.uniform(noise_key, (PROMPT_COUNT, blocks, SEG, HEADS), jnp.float32, 0.5, 1.5)
    leakage_rate = (leakage_rate * roughness).reshape(PROMPT_COUNT, PROMPT_LENGTH, HEADS)
    spike_locations = jax.random.randint(location_random_key, (PROMPT_COUNT, 2), 0, PROMPT_LENGTH)
    spike_magnitudes = jnp.log(jax.random.uniform(magnitude_random_key, (PROMPT_COUNT, 2), jnp.float32, 0.5, 0.8))
    token_position = jnp.arange(PROMPT_LENGTH)
    spike_contribution = jnp.sum(jnp.where(token_position[None, :, None] == spike_locations[:, None, :], spike_magnitudes[:, None, :], 0.0), axis=2)
    return spike_contribution[:, :, None] - leakage_rate


def draw_new_value(key, part):
    base = jnp.clip(jax.random.normal(key, (PROMPT_COUNT, HEADS, HEAD_DIM), jnp.float32), -6.0, 6.0)
    channel = jnp.arange(HEAD_DIM).astype(jnp.float32) / (HEAD_DIM - 1)
    rising = jnp.exp(jnp.log(10.0) * channel)
    return (base * rising).reshape(PROMPT_COUNT, HEADS * HEAD_DIM).astype(jnp.bfloat16)


def block_levels(key, shape, pieces, smallest, high):
    level, own = 1.0, jax.random.fold_in(key, 6)
    for dim, blocks in pieces:
        steps = jnp.exp(jax.random.uniform(jax.random.fold_in(own, dim), (blocks,), jnp.float32, smallest / len(pieces), high / len(pieces)))
        level = level * jnp.repeat(steps, shape[dim] // blocks).reshape([-1 if axis == dim else 1 for axis in range(len(shape))])
    return level


def gaussian(stream_key, dims, spread, limit, shards=(), kind=jnp.bfloat16):
    drawn = jax.random.normal(stream_key, dims, jnp.float32) * spread
    if len(shards) > 0:
        drawn = block_levels(stream_key, dims, shards, -0.22, 0.18) * drawn
    return jnp.clip(drawn, min=-limit, max=limit).astype(kind)


def setup_inputs(seed: int = 0) -> dict:
    splits = jax.random.split(jax.random.key(seed), 16)
    hidden_in = gaussian(splits[0], (PROMPT_COUNT, PROMPT_LENGTH, D), 1.0, 6.0, ((1, 32),))
    w_value = gaussian(splits[1], (D, HEADS * HEAD_DIM), D ** -0.5, 0.125, ((1, 4),))
    w_key = gaussian(splits[2], (D, GROUPS * STATE), D ** -0.5, 0.125, ((1, 4),))
    w_step = gaussian(splits[3], (D, HEADS), D ** -0.5, 0.125)
    conv_value = gaussian(splits[4], (KERNEL, HEADS * HEAD_DIM), KERNEL ** -0.5, 3.0, ((1, 4),))
    conv_key = gaussian(splits[5], (KERNEL, GROUPS * STATE), KERNEL ** -0.5, 3.0, ((1, 4),))
    step_bias = jnp.clip(-3.0 + 2.0 * jax.random.uniform(splits[6], (HEADS,), jnp.float32) ** block_levels(splits[6], (HEADS,), ((0, 4),), -0.2, 0.2), -3.0, -1.0)
    decay_rate = draw_decay_rate(jax.random.fold_in(splits[15], 71), 0)
    decay_jump = draw_decay_jump(jax.random.fold_in(splits[15], 71), 0)
    new_value = draw_new_value(jax.random.fold_in(splits[15], 71), 0)
    new_key = gaussian(splits[10], (PROMPT_COUNT, GROUPS * STATE), 1.0, 6.0, ((1, 4),))
    new_query = gaussian(splits[11], (PROMPT_COUNT, GROUPS * STATE), 1.0, 6.0, ((1, 4),))
    new_gate = gaussian(splits[12], (PROMPT_COUNT, HEADS * HEAD_DIM), 1.0, 6.0, ((1, 4),))
    new_step = gaussian(splits[13], (PROMPT_COUNT, HEADS), 1.0, 6.0, ((1, 4),), jnp.float32)
    read_gain = jnp.clip(1.0 + 0.18 * jax.random.normal(splits[14], (HEADS * HEAD_DIM,), jnp.float32), 0.099609375, 1.8984375).astype(jnp.bfloat16)
    return dict(hidden_in=hidden_in, w_value=w_value, w_key=w_key, w_step=w_step, conv_value=conv_value, conv_key=conv_key, step_bias=step_bias, decay_rate=decay_rate, decay_jump=decay_jump, new_value=new_value, new_key=new_key, new_query=new_query, new_gate=new_gate, new_step=new_step, read_gain=read_gain)


EPSILON = 1e-05

def causal_mix(padded_rows, conv_taps):
    tap_count = conv_taps.shape[0]
    length = padded_rows.shape[-2] - tap_count + 1
    running = jnp.zeros(padded_rows.shape[:-2] + (length, padded_rows.shape[-1]), jnp.float32)
    for tap_index in range(tap_count):
        running = running + padded_rows[..., tap_index:tap_index + length, :].astype(jnp.float32) * conv_taps[tap_index].astype(jnp.float32)
    return running

def reference(hidden_in, w_value, w_key, w_step, conv_value, conv_key, step_bias, decay_rate, decay_jump, new_value, new_key, new_query, new_gate, new_step, read_gain):
    per_group = HEADS // GROUPS
    value_cols = HEADS * HEAD_DIM
    conv_taps = jnp.concatenate([conv_value, conv_key], axis=1)

    def prompt_state(seq_pair):
        seq_rows, seq_jump = seq_pair
        proj_value = jnp.dot(seq_rows, w_value, preferred_element_type=jnp.float32).astype(jnp.bfloat16)
        proj_key = jnp.dot(seq_rows, w_key, preferred_element_type=jnp.float32).astype(jnp.bfloat16)
        proj_step = jnp.dot(seq_rows, w_step, preferred_element_type=jnp.float32).astype(jnp.bfloat16)
        joined_cols = jnp.concatenate([proj_value, proj_key], axis=1)
        padded_rows = jnp.pad(joined_cols, ((KERNEL - 1, 0), (0, 0)))
        mixed_rows = jax.nn.silu(causal_mix(padded_rows, conv_taps))
        step_size = jax.nn.softplus(proj_step.astype(jnp.float32) + step_bias)
        log_decay = seq_jump - decay_rate * step_size
        decay_after = lax.optimization_barrier(jnp.sum(log_decay, axis=0, keepdims=True)) - jnp.cumsum(log_decay, axis=0)
        weight = step_size * jnp.exp(decay_after)
        values = mixed_rows[:, :value_cols].reshape(PROMPT_LENGTH, GROUPS, per_group, HEAD_DIM) * weight.reshape(PROMPT_LENGTH, GROUPS, per_group)[..., None]
        keys = mixed_rows[:, value_cols:].reshape(PROMPT_LENGTH, GROUPS, STATE)
        states = jnp.einsum('lgep,lgn->gepn', values, keys, precision=lax.Precision.HIGHEST)
        return states.reshape(HEADS, HEAD_DIM, STATE)
    final_state = lax.map(prompt_state, (hidden_in, decay_jump))
    cache_state = final_state.astype(jnp.bfloat16)
    new_size = jax.nn.softplus(new_step + step_bias)
    keep_share = jnp.exp(-decay_rate * new_size)
    query = new_query.astype(jnp.float32).reshape(PROMPT_COUNT, GROUPS, STATE)
    own_key = new_key.astype(jnp.float32).reshape(PROMPT_COUNT, GROUPS, STATE)
    state_read = jnp.einsum('sgepn,sgn->sgep', final_state.reshape(PROMPT_COUNT, GROUPS, per_group, HEAD_DIM, STATE), query, precision=lax.Precision.HIGHEST)
    key_match = lax.optimization_barrier(jnp.sum(own_key * query, axis=-1))
    own_value = new_value.astype(jnp.float32).reshape(PROMPT_COUNT, GROUPS, per_group, HEAD_DIM)
    size_grid = new_size.reshape(PROMPT_COUNT, GROUPS, per_group)
    keep_grid = keep_share.reshape(PROMPT_COUNT, GROUPS, per_group)
    raw_read = keep_grid[..., None] * state_read + size_grid[..., None] * own_value * key_match[:, :, None, None]
    gated = raw_read.reshape(PROMPT_COUNT, GROUPS, per_group * HEAD_DIM) * jax.nn.silu(new_gate.astype(jnp.float32)).reshape(PROMPT_COUNT, GROUPS, per_group * HEAD_DIM)
    normed = gated * lax.rsqrt(lax.optimization_barrier(jnp.mean(gated * gated, axis=-1, keepdims=True)) + EPSILON)
    read_out = (normed.reshape(PROMPT_COUNT, HEADS * HEAD_DIM) * read_gain.astype(jnp.float32)).astype(jnp.bfloat16)
    return (cache_state, read_out.reshape(PROMPT_COUNT, HEADS, HEAD_DIM))
```

```python
import jax
import jax.numpy as jnp
from jax import lax
from jax.experimental import pallas as pl
from jax.experimental.pallas import tpu as pltpu
from jax.sharding import PartitionSpec as P

HEAD_DIM = 64
STATE = 128


EPSILON = 1e-05


def shifted(value, axis, steps):
    count = lax.axis_size(axis)
    leading, last = (max(0, -steps), min(count, count - steps))
    return lax.ppermute(value, axis, [(source, source + steps) for source in range(leading, last)])


def causal_mix(padded_rows, conv_taps):
    tap_count = conv_taps.shape[0]
    length = padded_rows.shape[-2] - tap_count + 1
    running = jnp.zeros(padded_rows.shape[:-2] + (length, padded_rows.shape[-1]), jnp.float32)
    for tap_index in range(tap_count):
        running = running + padded_rows[..., tap_index : tap_index + length, :].astype(
            jnp.float32
        ) * conv_taps[tap_index].astype(jnp.float32)
    return running


def block_states(mixed_rows, weight, value_cols, groups_dev):
    seq_count, row_count, heads_dev = weight.shape
    per_group = heads_dev // groups_dev
    values = (
        mixed_rows[:, :, :value_cols].reshape(seq_count, row_count, groups_dev, per_group, HEAD_DIM)
        * weight.reshape(seq_count, row_count, groups_dev, per_group)[..., None]
    )
    keys = mixed_rows[:, :, value_cols:].reshape(seq_count, row_count, groups_dev, STATE)
    states = jnp.einsum("slgep,slgn->sgepn", values, keys, precision=lax.Precision.HIGHEST)
    return states.reshape(seq_count, heads_dev, HEAD_DIM, STATE)


def general(
    hidden_in,
    w_value,
    w_key,
    w_step,
    conv_value,
    conv_key,
    step_bias,
    decay_rate,
    decay_jump,
    new_value,
    new_key,
    new_query,
    new_gate,
    new_step,
    read_gain,
):
    sp_count = lax.axis_size("sp")
    sp_index = lax.axis_index("sp")
    tp_index = lax.axis_index("tp")
    heads_dev = step_bias.shape[0]
    value_cols = w_value.shape[1]
    key_cols = w_key.shape[1]
    groups_dev = key_cols // STATE
    per_group = heads_dev // groups_dev
    kernel_taps = conv_value.shape[0]
    seq_count = hidden_in.shape[0]
    share = HEAD_DIM // sp_count
    own_step = lax.dynamic_slice_in_dim(w_step, tp_index * heads_dev, heads_dev, 1)
    w_joined = jnp.concatenate([w_value, w_key, own_step], axis=1)
    projected = jnp.einsum(
        "tfy,yz->tfz",
        lax.all_gather(hidden_in, "tp", axis=1, tiled=True),
        w_joined,
        preferred_element_type=jnp.float32,
    ).astype(jnp.bfloat16)
    seg_rows = projected.shape[1]
    proj_pair = projected[:, :, : value_cols + key_cols]
    proj_step = projected[:, :, value_cols + key_cols :]
    step_size = jax.nn.softplus(proj_step.astype(jnp.float32) + step_bias)
    log_decay = decay_jump - decay_rate * step_size
    conv_taps = jnp.concatenate([conv_value, conv_key], axis=1)
    edge_rows = shifted(proj_pair[:, seg_rows - (kernel_taps - 1) :, :], "sp", 1)
    mixed_rows = jax.nn.silu(causal_mix(jnp.concatenate([edge_rows, proj_pair], axis=1), conv_taps))
    seg_total = jnp.sum(log_decay, axis=1)
    decay_after = seg_total[:, None, :] - jnp.cumsum(log_decay, axis=1)
    seg_states = block_states(mixed_rows, step_size * jnp.exp(decay_after), value_cols, groups_dev)
    tiled_totals = jnp.broadcast_to(
        seg_total[:, None, :, None], (seq_count, 1, heads_dev, sp_count)
    )
    got_states, got_totals = (
        lax.all_to_all(seg_states[:, None], "sp", split_axis=3, concat_axis=1, tiled=True),
        lax.all_to_all(tiled_totals, "sp", split_axis=3, concat_axis=1, tiled=True),
    )
    got_totals = got_totals[..., 0]
    tail_decay = jnp.sum(got_totals, axis=1, keepdims=True) - jnp.cumsum(got_totals, axis=1)
    final_state = jnp.einsum(
        "sjh,sjhpn->shpn", jnp.exp(tail_decay), got_states, precision=lax.Precision.HIGHEST
    )
    cache_state = final_state.astype(jnp.bfloat16)
    new_size = jax.nn.softplus(new_step + step_bias)
    keep_share = jnp.exp(-decay_rate * new_size)
    query = new_query.astype(jnp.float32).reshape(seq_count, groups_dev, STATE)
    own_key = new_key.astype(jnp.float32).reshape(seq_count, groups_dev, STATE)
    key_match = jnp.sum(own_key * query, axis=-1)
    size_grid = new_size.reshape(seq_count, groups_dev, per_group)
    keep_grid = keep_share.reshape(seq_count, groups_dev, per_group)
    value_grid = new_value.astype(jnp.float32).reshape(seq_count, groups_dev, per_group, HEAD_DIM)
    gate_grid = jax.nn.silu(new_gate.astype(jnp.float32)).reshape(
        seq_count, groups_dev, per_group, HEAD_DIM
    )
    gain_grid = read_gain.astype(jnp.float32).reshape(groups_dev, per_group, HEAD_DIM)
    own_value = lax.dynamic_slice_in_dim(value_grid, sp_index * share, share, 3)
    own_gate = lax.dynamic_slice_in_dim(gate_grid, sp_index * share, share, 3)
    own_gain = lax.dynamic_slice_in_dim(gain_grid, sp_index * share, share, 2)
    state_read = jnp.einsum(
        "sgepn,sgn->sgep",
        final_state.reshape(seq_count, groups_dev, per_group, share, STATE),
        query,
        precision=lax.Precision.HIGHEST,
    )
    raw_read = (
        keep_grid[..., None] * state_read
        + size_grid[..., None] * own_value * key_match[:, :, None, None]
    )
    gated = raw_read * own_gate
    squares = lax.psum(jnp.sum(gated * gated, axis=(2, 3)), "sp")
    scale = lax.rsqrt(squares / (per_group * HEAD_DIM) + EPSILON)
    read_out = (gated * scale[:, :, None, None] * own_gain).astype(jnp.bfloat16)
    return (cache_state, read_out.reshape(seq_count, heads_dev, share))


MESH = pl.DeviceIdType.MESH
PIECES = 4
ROW_TILE = 64
EDGE = 16


def softplus(x):
    return jnp.maximum(x, 0.0) + jnp.log1p(jnp.exp(-jnp.abs(x)))


def flip(value, bit):
    return value + bit - 2 * bit * ((value // bit) % 2)


def mixer_kernel(
    hid, wv, wk, wstep, taps, bias_rate, jump, query, coef,
    state_out, read_out,
    rows, w_all, tall, jall, ball, qall, step_t, wx, proj, val, key, totals, stage, full, got, reads, read_got,
    hid_local, hid_send, hid_recv, w_local, edge_send, edge_recv, small_send, small_recv,
    y_send, x_send, z_send, w_recv, tot_send, tot_recv, st_send, st_recv, rd_send, rd_recv,
):
    sp, tp = lax.axis_index("sp"), lax.axis_index("tp")
    sp_count = lax.axis_size("sp")
    y, core = tp // 2, tp % 2
    far = 1 - y
    chips = 2 * sp_count
    seqs, part, width = hid.shape
    local = 2 * part
    depth = width // PIECES
    groups = w_all.shape[1]
    heads = jump.shape[1]
    share = 64 // sp_count
    per_share = stage.shape[3] // seqs
    quarter = sp % 4

    def xor_sp(bits):
        out, bit = sp, 1
        while bit < sp_count:
            if bits & bit:
                out = flip(out, bit)
            bit *= 2
        return out

    x_peer, z_peer, y_peer = (flip(sp, 1), tp), (flip(sp, 2), tp), (sp, flip(tp, 2))
    core_peer = (sp, flip(tp, 1))

    def chip_peer(r):
        return (xor_sp(r % sp_count), flip(tp, 2) if r >= sp_count else tp)

    def send(src, dst, send_sem, recv_sem, peer):
        return pltpu.make_async_remote_copy(
            src_ref=src, dst_ref=dst, send_sem=send_sem, recv_sem=recv_sem, device_id=peer, device_id_type=MESH
        )

    order = sp * 2 + y
    after = lax.rem(order + 1, chips)

    barrier = pltpu.get_barrier_semaphore()
    for r in range(1, chips):
        pl.semaphore_signal(barrier, inc=1, device_id=chip_peer(r), device_id_type=MESH)
    pl.semaphore_signal(barrier, inc=1, device_id=core_peer, device_id_type=MESH)
    before = lax.rem(order + chips - 1, chips)

    @pl.when(core == 0)
    def _():
        pl.semaphore_signal(
            barrier, inc=1, device_id=(before // 2, (before % 2) * 2 + 1), device_id_type=MESH
        )


    mine = pl.ds(pl.multiple_of(EDGE + core * part, 16), part)
    load_hid = [pltpu.make_async_copy(hid.at[s], rows.at[s, mine, :], hid_local.at[s]) for s in range(seqs)]
    load_w = [
        pltpu.make_async_copy(
            w.at[:, pl.ds(a * 128, 128)], w_all.at[y, a, half], w_local.at[a, half]
        )
        for a in range(groups)
        for half, w in enumerate((wv, wk))
    ]
    for c in load_hid + load_w:
        c.start()
    jall[y] = jump[:, :, pl.ds(pl.multiple_of(y * local, 128), local)]
    ball[y] = bias_rate[...]
    tall[y] = taps[...]
    qall[y] = query[...]
    reads[...] = jnp.zeros(reads.shape, jnp.float32)
    pl.semaphore_wait(barrier, chips + core)

    send_hid = [
        send(hid.at[s], rows.at[s, mine, :], hid_send.at[s], hid_recv.at[s], core_peer) for s in range(seqs)
    ]
    theirs = pl.ds(pl.multiple_of(far * local, 128), local)
    send_small = [
        send(jump.at[:, :, theirs], jall.at[y], small_send.at[0], small_recv.at[0], y_peer),
        send(bias_rate, ball.at[y], small_send.at[1], small_recv.at[1], y_peer),
        send(taps, tall.at[y], small_send.at[2], small_recv.at[2], y_peer),
        send(query, qall.at[y], small_send.at[3], small_recv.at[3], y_peer),
    ]
    count = 2 * PIECES
    diag = groups - 1 - quarter
    first, second = (3 * count) // 8, (6 * count) // 8
    y_list = [(quarter, chunk, 0) for chunk in range(count)] + [(diag, chunk, 3) for chunk in range(second, count)]
    send_y = [
        send(
            (wv, wk)[chunk % 2].at[pl.ds((chunk // 2) * depth, depth), pl.ds(pl.multiple_of(a * 128, 128), 128)],
            w_all.at[y, a, chunk % 2, pl.ds((chunk // 2) * depth, depth), :],
            y_send.at[n], w_recv.at[rel, chunk], y_peer,
        )
        for n, (a, chunk, rel) in enumerate(y_list)
    ]
    edge = [
        send(
            hid.at[:, pl.ds(part - EDGE, EDGE), :], rows.at[:, pl.ds(0, EDGE), :], edge_send.at[c], edge_recv,
            (after // 2, (after % 2) * 2 + c),
        )
        for c in range(2)
    ]

    @pl.when(core == 1)
    def _():
        for c in edge:
            c.start()

    for c in send_hid + send_y[:1] + send_small + send_y[1:]:
        c.start()

    def w_copy(a, chunk, send_sem, rel, peer):
        block = w_all.at[
            far, a, chunk % 2, pl.ds(pl.multiple_of((chunk // 2) * depth, depth), depth), :
        ]
        return send(block, block, send_sem, w_recv.at[rel, chunk], peer)

    def wait_chunk(rel, a, chunk):
        w_copy(a, chunk, y_send.at[0], rel, y_peer).wait_recv()

    def relay(chunk):
        wait_chunk(0, quarter, chunk)
        w_copy(quarter, chunk, x_send.at[chunk], 1, x_peer).start()
        w_copy(quarter, chunk, z_send.at[chunk], 2, z_peer).start()

    qx, qz = flip(quarter, 1), flip(quarter, 2)

    def relay_diag(n):
        wait_chunk(1, qx, n)
        w_copy(qx, n, z_send.at[count + n], 3, z_peer).start()
        wait_chunk(2, qz, first + n)
        w_copy(qz, first + n, x_send.at[count + n], 3, x_peer).start()

    for c in load_hid:
        c.wait()
    for c in send_hid:
        c.wait_recv()
    relay(0)
    for s in range(seqs):
        step_t[s] = (
            lax.dot_general(
                wstep[...], rows[s, EDGE:, :], (((1,), (1,)), ((), ())), preferred_element_type=jnp.float32
            )
            .astype(jnp.bfloat16)
            .astype(jnp.float32)
        )
    for c in send_small:
        c.wait_recv()
    decays, sizes = [], []
    for yb in range(2):
        for s in range(seqs):
            raw = step_t[s, pl.ds(pl.multiple_of((2 * yb + core) * heads, 8), heads), :]
            one = softplus(raw + ball[yb, :, 0:1])
            sizes.append(one)
            decays.append(jall[yb, s] - ball[yb, :, 1:2] * one)
    size = jnp.concatenate(sizes, axis=0)
    decay = jnp.concatenate(decays, axis=0)
    column = lax.broadcasted_iota(jnp.int32, (heads, 128), 1)
    packed = jnp.zeros((heads, 128), jnp.float32)
    for n, one in enumerate(decays):
        packed = jnp.where(column == n, jnp.sum(one, axis=1, keepdims=True), packed)
    totals[0] = packed
    relay(1)
    send_tot = [
        send(totals.at[0], totals.at[r], tot_send.at[r], tot_recv.at[r], chip_peer(r)) for r in range(1, chips)
    ]
    for c in send_tot:
        c.start()
    spot = lax.broadcasted_iota(jnp.int32, decay.shape, 1)
    suffix = jnp.where(spot < local - 1, pltpu.roll(decay, local - 1, 1), 0.0)
    shift = 1
    while shift < local:
        suffix = suffix + jnp.where(spot < local - shift, pltpu.roll(suffix, local - shift, 1), 0.0)
        shift *= 2
    edge[0].wait_recv()

    @pl.when(order == 0)
    def _():
        rows[:, 0:EDGE, :] = jnp.zeros((seqs, EDGE, width), rows.dtype)

    relay(2)
    later = jnp.zeros((heads, 128), jnp.float32)
    for r in range(1, chips):
        send_tot[r - 1].wait_recv()
        source = xor_sp(r % sp_count) * 2 + (far if r >= sp_count else y)
        later = later + totals[r] * jnp.where(source > order, 1.0, 0.0)
    later = jnp.concatenate([later[:, n : n + 1] for n in range(len(decays))], axis=0)
    weight_t = (size * jnp.exp(suffix + later)).T
    lane = lax.broadcasted_iota(jnp.int32, (local, 128), 1)
    for yb in range(2):
        for s in range(seqs):
            for a in range(groups):
                at = (yb * seqs + s) * heads + 2 * a
                wx[yb, s, a] = jnp.where(lane < 64, weight_t[:, at : at + 1], weight_t[:, at + 1 : at + 2])
    for c in load_w:
        c.wait()

    def step(slot, block, a, s):
        proj[...] = (
            jnp.dot(rows[s], jnp.concatenate([w_all[block, a, 0], w_all[block, a, 1]], axis=1), preferred_element_type=jnp.float32)
            .astype(jnp.bfloat16)
            .astype(jnp.float32)
        )
        tap = tall[block, a]

        def mix(i, carry):
            base = pl.multiple_of(i * ROW_TILE, ROW_TILE)
            span = proj[pl.ds(base + 8, ROW_TILE + 8), :]
            acc = span[5 : 5 + ROW_TILE] * tap[0:1]
            for k in range(1, 4):
                acc = acc + span[5 + k : 5 + k + ROW_TILE] * tap[k : k + 1]
            acc = acc / (1.0 + jnp.exp(-acc))
            here = pl.ds(base, ROW_TILE)
            val[here, :] = (acc[:, :128] * wx[block, s, a, here, :]).astype(jnp.bfloat16)
            key[here, :] = acc[:, 128:].astype(jnp.bfloat16)
            return carry

        lax.fori_loop(0, local // ROW_TILE, mix, 0)
        state = lax.dot_general(
            val[...], key[...], (((0,), (0,)), ((), ())), preferred_element_type=jnp.float32
        )
        per = state.shape[0] // 64
        parts = jnp.swapaxes(state.reshape(per, sp_count, share, 128), 0, 1).reshape(sp_count, per_share, 128)
        here = pl.ds(pl.multiple_of(s * per_share, per_share), per_share)
        stage[slot, a, :, here, :] = parts.astype(jnp.bfloat16)
        line = a * seqs + s
        read = lax.dot_general(
            qall[block, line], state, (((1,), (1,)), ((), ())),
            precision=lax.Precision.HIGHEST, preferred_element_type=jnp.float32,
        )
        reads[slot] = jnp.where(lax.broadcasted_iota(jnp.int32, read.shape, 0) == line, read, reads[slot])
        if slot == 0:
            full[a, :, here, :] = parts

    def send_states(slot, a, peers):
        for r in peers:
            send(
                stage.at[slot, a, xor_sp(r % sp_count)], got.at[r - 1, a], st_send, st_recv, chip_peer(r)
            ).start()

    ready = 3

    def own_block(j, carry):
        a, s = j // seqs, j % seqs

        @pl.when(j < count - ready)
        def _():
            relay(j + ready)

        @pl.when(j >= count - ready)
        def _():
            relay_diag(j - (count - ready))

        step(0, y, a, s)

        @pl.when(s == seqs - 1)
        def _():
            send_states(0, a, range(1, sp_count))

        return carry

    lax.fori_loop(0, groups * seqs, own_block, 0)

    def send_reads(slot, r):
        return send(reads.at[slot], read_got.at[r], rd_send.at[r], rd_recv.at[r], chip_peer(r))

    waits = {
        1: list(range(first, count)),
        2: list(range(first)) + list(range(second, count)),
        3: list(range(count)),
    }

    def far_block(j, carry):
        k, s = j // seqs, j % seqs
        a = (quarter % 2 + k % 2) % 2 + 2 * ((quarter // 2 + k // 2) % 2)
        for rel, chunks in waits.items():

            @pl.when(j == rel * seqs)
            def _():
                for chunk in chunks:
                    wait_chunk(rel, a, chunk)

        @pl.when(j == 1)
        def _():
            for r in range(1, sp_count):
                send_reads(0, r).start()

        step(1, far, a, s)

        @pl.when(s == seqs - 1)
        def _():
            send_states(1, a, range(sp_count, chips))

        return carry

    lax.fori_loop(0, groups * seqs, far_block, 0)

    send_rd = [send_reads(r // sp_count, r) for r in range(1, chips)]
    for c in send_rd[sp_count - 1 :]:
        c.start()
    everything = send(got, got, st_send, st_recv, y_peer)
    everything.wait_recv()
    for a in range(groups):
        final = full[a, sp]
        for r in range(chips - 1):
            final = final + got[r, a].astype(jnp.float32)
        state_out[a] = final
    read = reads[0]
    for r in range(1, chips):
        send_rd[r - 1].wait_recv()
        read = read + read_got[r]
    gated = coef[0] * read + coef[1]
    mean = jnp.mean(gated * gated, axis=1, keepdims=True)
    read_out[...] = gated * lax.rsqrt(mean + EPSILON) * coef[2]
    @pl.when(core == 1)
    def _():
        for c in edge:
            c.wait_send()

    for c in send_hid + send_small + send_y + send_tot + send_rd + [everything]:
        c.wait_send()
    for n in range(count):
        w_copy(quarter, n, x_send.at[n], 1, x_peer).wait_send()
        w_copy(quarter, n, z_send.at[n], 2, z_peer).wait_send()
    for n in range(first):
        w_copy(qx, n, z_send.at[count + n], 3, z_peer).wait_send()
        w_copy(qz, n, x_send.at[count + n], 3, x_peer).wait_send()


def per_device(
    hidden_in, w_value, w_key, w_step, conv_value, conv_key, step_bias, decay_rate, decay_jump,
    new_value, new_key, new_query, new_gate, new_step, read_gain,
):
    sp_count, tp_count = lax.axis_size("sp"), lax.axis_size("tp")
    heads = step_bias.shape[0]
    groups = w_key.shape[1] // STATE
    seqs, part, width = hidden_in.shape
    per = heads // groups
    share = HEAD_DIM // sp_count
    if not (tp_count == 4 and groups == 4 and share == 8 and per == 2 and seqs == 2 and part % 64 == 0):
        return general(
            hidden_in, w_value, w_key, w_step, conv_value, conv_key, step_bias, decay_rate, decay_jump,
            new_value, new_key, new_query, new_gate, new_step, read_gain,
        )
    f32 = jnp.float32
    sp_index = lax.axis_index("sp")
    local = 2 * part
    tap_count = conv_value.shape[0]
    taps = jnp.concatenate(
        [conv_value.reshape(tap_count, groups, 128), conv_key.reshape(tap_count, groups, 128)], axis=2
    )
    taps = jnp.pad(jnp.swapaxes(taps, 0, 1).astype(f32), ((0, 0), (0, 8 - tap_count), (0, 0)))
    bias_rate = jnp.pad(jnp.stack([step_bias, decay_rate], axis=1), ((0, 0), (0, 126)))

    def lines_of(x):
        return jnp.swapaxes(x.astype(f32).reshape(seqs, groups, -1), 0, 1)

    def per_channel(x):
        return jnp.repeat(lines_of(x), HEAD_DIM, axis=2)

    query = lines_of(new_query)
    key_match = jnp.sum(lines_of(new_key) * query, axis=-1, keepdims=True)
    new_size = jax.nn.softplus(new_step + step_bias)
    gate = jax.nn.silu(lines_of(new_gate))
    coef = jnp.stack(
        [
            per_channel(jnp.exp(-decay_rate * new_size)) * gate,
            per_channel(new_size) * lines_of(new_value) * key_match * gate,
            jnp.broadcast_to(read_gain.astype(f32).reshape(groups, 1, per * HEAD_DIM), gate.shape),
        ]
    ).reshape(3, groups * seqs, per * HEAD_DIM)
    query = jnp.broadcast_to(query.reshape(groups * seqs, 1, STATE), (groups * seqs, 8, STATE))
    chips = 2 * sp_count
    bf16 = jnp.bfloat16
    block = seqs * per * share
    vmem, anyspace = pl.BlockSpec(memory_space=pltpu.VMEM), pl.BlockSpec(memory_space=pl.ANY)
    dma = pltpu.SemaphoreType.DMA
    count = 2 * PIECES
    state, read = pl.pallas_call(
        mixer_kernel,
        out_shape=(
            jax.ShapeDtypeStruct((groups, block, 128), f32),
            jax.ShapeDtypeStruct((groups * seqs, 128), f32),
        ),
        in_specs=[anyspace] * 3 + [vmem] * 6,
        out_specs=(vmem, vmem),
        scratch_shapes=[
            pltpu.VMEM((seqs, EDGE + local, width), bf16),
            pltpu.VMEM((2, groups, 2, width, 128), bf16),
            pltpu.VMEM((2, groups, 8, 256), f32),
            pltpu.VMEM((2, seqs, heads, local), f32),
            pltpu.VMEM((2, heads, 128), f32),
            pltpu.VMEM((2, groups * seqs, 8, STATE), f32),
            pltpu.VMEM((seqs, 4 * heads, local), f32),
            pltpu.VMEM((2, seqs, groups, local, 128), f32),
            pltpu.VMEM((EDGE + local, 256), f32),
            pltpu.VMEM((local, 128), bf16),
            pltpu.VMEM((local, 128), bf16),
            pltpu.VMEM((chips, heads, 128), f32),
            pltpu.VMEM((2, groups, sp_count, block, 128), bf16),
            pltpu.VMEM((groups, sp_count, block, 128), f32),
            pltpu.VMEM((chips - 1, groups, block, 128), bf16),
            pltpu.VMEM((2, groups * seqs, 128), f32),
            pltpu.VMEM((chips, groups * seqs, 128), f32),
            dma((seqs,)), dma((seqs,)), dma((seqs,)), dma((groups, 2)), dma((2,)), dma, dma((4,)), dma((4,)),
            dma((2 * count,)), dma((2 * count,)), dma((2 * count,)), dma((4, count)),
            dma((chips,)), dma((chips,)), dma, dma, dma((chips,)), dma((chips,)),
        ],
        compiler_params=pltpu.CompilerParams(
            collective_id=0, has_side_effects=True, vmem_limit_bytes=60 * 1024 * 1024
        ),
    )(
        hidden_in, w_value, w_key, jnp.swapaxes(w_step, 0, 1), taps, bias_rate,
        jnp.swapaxes(decay_jump, 1, 2), query, coef,
    )

    state = jnp.swapaxes(state.reshape(groups, seqs, per, share, STATE), 0, 1)
    read = lax.dynamic_slice_in_dim(read.reshape(groups, seqs, per, HEAD_DIM), sp_index * share, share, 3)
    read = jnp.swapaxes(read, 0, 1)
    return (
        state.reshape(seqs, heads, share, STATE).astype(bf16),
        read.reshape(seqs, heads, share).astype(bf16),
    )


def solution(mesh):
    return jax.shard_map(
        per_device,
        mesh=mesh,
        in_specs=(
            P(None, ("sp", "tp"), None),
            P(None, "tp"),
            P(None, "tp"),
            P(),
            P(None, "tp"),
            P(None, "tp"),
            P("tp"),
            P("tp"),
            P(None, "sp", "tp"),
            P(None, "tp"),
            P(None, "tp"),
            P(None, "tp"),
            P(None, "tp"),
            P(None, "tp"),
            P("tp"),
        ),
        out_specs=(P(None, "tp", "sp", None), P(None, "tp", "sp")),
        check_vma=False,
    )
```

```python
import jax
import jax.numpy as jnp
from jax import lax
from jax.experimental import pallas as pl
from jax.experimental.pallas import tpu as pltpu
from jax.sharding import PartitionSpec as P

HEAD_DIM = 64
STATE = 128


EPSILON = 1e-05


def shifted(value, axis, steps):
    count = lax.axis_size(axis)
    leading, last = (max(0, -steps), min(count, count - steps))
    return lax.ppermute(value, axis, [(source, source + steps) for source in range(leading, last)])


def causal_mix(padded_rows, conv_taps):
    tap_count = conv_taps.shape[0]
    length = padded_rows.shape[-2] - tap_count + 1
    running = jnp.zeros(padded_rows.shape[:-2] + (length, padded_rows.shape[-1]), jnp.float32)
    for tap_index in range(tap_count):
        running = running + padded_rows[..., tap_index : tap_index + length, :].astype(
            jnp.float32
        ) * conv_taps[tap_index].astype(jnp.float32)
    return running


def block_states(mixed_rows, weight, value_cols, groups_dev):
    seq_count, row_count, heads_dev = weight.shape
    per_group = heads_dev // groups_dev
    values = (
        mixed_rows[:, :, :value_cols].reshape(seq_count, row_count, groups_dev, per_group, HEAD_DIM)
        * weight.reshape(seq_count, row_count, groups_dev, per_group)[..., None]
    )
    keys = mixed_rows[:, :, value_cols:].reshape(seq_count, row_count, groups_dev, STATE)
    states = jnp.einsum("slgep,slgn->sgepn", values, keys, precision=lax.Precision.HIGHEST)
    return states.reshape(seq_count, heads_dev, HEAD_DIM, STATE)


def general(
    hidden_in,
    w_value,
    w_key,
    w_step,
    conv_value,
    conv_key,
    step_bias,
    decay_rate,
    decay_jump,
    new_value,
    new_key,
    new_query,
    new_gate,
    new_step,
    read_gain,
):
    sp_count = lax.axis_size("sp")
    sp_index = lax.axis_index("sp")
    tp_index = lax.axis_index("tp")
    heads_dev = step_bias.shape[0]
    value_cols = w_value.shape[1]
    key_cols = w_key.shape[1]
    groups_dev = key_cols // STATE
    per_group = heads_dev // groups_dev
    kernel_taps = conv_value.shape[0]
    seq_count = hidden_in.shape[0]
    share = HEAD_DIM // sp_count
    own_step = lax.dynamic_slice_in_dim(w_step, tp_index * heads_dev, heads_dev, 1)
    w_joined = jnp.concatenate([w_value, w_key, own_step], axis=1)
    projected = jnp.einsum(
        "tfy,yz->tfz",
        lax.all_gather(hidden_in, "tp", axis=1, tiled=True),
        w_joined,
        preferred_element_type=jnp.float32,
    ).astype(jnp.bfloat16)
    seg_rows = projected.shape[1]
    proj_pair = projected[:, :, : value_cols + key_cols]
    proj_step = projected[:, :, value_cols + key_cols :]
    step_size = jax.nn.softplus(proj_step.astype(jnp.float32) + step_bias)
    log_decay = decay_jump - decay_rate * step_size
    conv_taps = jnp.concatenate([conv_value, conv_key], axis=1)
    edge_rows = shifted(proj_pair[:, seg_rows - (kernel_taps - 1) :, :], "sp", 1)
    mixed_rows = jax.nn.silu(causal_mix(jnp.concatenate([edge_rows, proj_pair], axis=1), conv_taps))
    seg_total = jnp.sum(log_decay, axis=1)
    decay_after = seg_total[:, None, :] - jnp.cumsum(log_decay, axis=1)
    seg_states = block_states(mixed_rows, step_size * jnp.exp(decay_after), value_cols, groups_dev)
    tiled_totals = jnp.broadcast_to(
        seg_total[:, None, :, None], (seq_count, 1, heads_dev, sp_count)
    )
    got_states, got_totals = (
        lax.all_to_all(seg_states[:, None], "sp", split_axis=3, concat_axis=1, tiled=True),
        lax.all_to_all(tiled_totals, "sp", split_axis=3, concat_axis=1, tiled=True),
    )
    got_totals = got_totals[..., 0]
    tail_decay = jnp.sum(got_totals, axis=1, keepdims=True) - jnp.cumsum(got_totals, axis=1)
    final_state = jnp.einsum(
        "sjh,sjhpn->shpn", jnp.exp(tail_decay), got_states, precision=lax.Precision.HIGHEST
    )
    cache_state = final_state.astype(jnp.bfloat16)
    new_size = jax.nn.softplus(new_step + step_bias)
    keep_share = jnp.exp(-decay_rate * new_size)
    query = new_query.astype(jnp.float32).reshape(seq_count, groups_dev, STATE)
    own_key = new_key.astype(jnp.float32).reshape(seq_count, groups_dev, STATE)
    key_match = jnp.sum(own_key * query, axis=-1)
    size_grid = new_size.reshape(seq_count, groups_dev, per_group)
    keep_grid = keep_share.reshape(seq_count, groups_dev, per_group)
    value_grid = new_value.astype(jnp.float32).reshape(seq_count, groups_dev, per_group, HEAD_DIM)
    gate_grid = jax.nn.silu(new_gate.astype(jnp.float32)).reshape(
        seq_count, groups_dev, per_group, HEAD_DIM
    )
    gain_grid = read_gain.astype(jnp.float32).reshape(groups_dev, per_group, HEAD_DIM)
    own_value = lax.dynamic_slice_in_dim(value_grid, sp_index * share, share, 3)
    own_gate = lax.dynamic_slice_in_dim(gate_grid, sp_index * share, share, 3)
    own_gain = lax.dynamic_slice_in_dim(gain_grid, sp_index * share, share, 2)
    state_read = jnp.einsum(
        "sgepn,sgn->sgep",
        final_state.reshape(seq_count, groups_dev, per_group, share, STATE),
        query,
        precision=lax.Precision.HIGHEST,
    )
    raw_read = (
        keep_grid[..., None] * state_read
        + size_grid[..., None] * own_value * key_match[:, :, None, None]
    )
    gated = raw_read * own_gate
    squares = lax.psum(jnp.sum(gated * gated, axis=(2, 3)), "sp")
    scale = lax.rsqrt(squares / (per_group * HEAD_DIM) + EPSILON)
    read_out = (gated * scale[:, :, None, None] * own_gain).astype(jnp.bfloat16)
    return (cache_state, read_out.reshape(seq_count, heads_dev, share))


MESH = pl.DeviceIdType.MESH
PIECES = 4
EDGE = 16
TIP = 8


def softplus(x):
    return jnp.maximum(x, 0.0) + jnp.log1p(jnp.exp(-jnp.abs(x)))


def flip(value, bit):
    return value + bit - 2 * bit * ((value // bit) % 2)


def mixer_kernel(
    hid, wv, wk, wstep, cv, ck, jump, newv, newk, newq, newg, bias, rate, newstep,
    state_out, read_out,
    rows, w_all, wst, ctap, tall, jall, ball, nraw, qraw, qall, coef, step_t, wrow, proj, sfull, fac, totals,
    stage, full, got, reads, read_got,
    hid_local, hid_send, hid_recv, w_local, small_local, edge_send, edge_recv, small_send, small_recv,
    y_send, x_send, z_send, w_recv, tot_send, tot_recv, st_send, st_recv, rd_send, rd_recv,
):
    sp, tp = lax.axis_index("sp"), lax.axis_index("tp")
    sp_count = lax.axis_size("sp")
    y, core = tp // 2, tp % 2
    far = 1 - y
    chips = 2 * sp_count
    seqs, part, width = hid.shape
    local = 2 * part
    depth = width // PIECES
    groups = w_all.shape[1]
    heads = jump.shape[1]
    lines = groups * seqs
    share = 64 // sp_count
    per_share = stage.shape[3] // seqs
    quarter = sp % 4
    f32, bf16 = jnp.float32, jnp.bfloat16

    def xor_sp(bits):
        out, bit = sp, 1
        while bit < sp_count:
            if bits & bit:
                out = flip(out, bit)
            bit *= 2
        return out

    x_peer, z_peer, y_peer = (flip(sp, 1), tp), (flip(sp, 2), tp), (sp, flip(tp, 2))
    core_peer = (sp, flip(tp, 1))

    def chip_peer(r):
        return (xor_sp(r % sp_count), flip(tp, 2) if r >= sp_count else tp)

    def send(src, dst, send_sem, recv_sem, peer):
        return pltpu.make_async_remote_copy(
            src_ref=src, dst_ref=dst, send_sem=send_sem, recv_sem=recv_sem, device_id=peer, device_id_type=MESH
        )

    order = sp * 2 + y
    after = lax.rem(order + 1, chips)
    before = lax.rem(order + chips - 1, chips)

    barrier = pltpu.get_barrier_semaphore()
    for r in range(1, chips):
        pl.semaphore_signal(barrier, inc=1, device_id=chip_peer(r), device_id_type=MESH)
    pl.semaphore_signal(barrier, inc=1, device_id=core_peer, device_id_type=MESH)

    @pl.when(core == 0)
    def _():
        pl.semaphore_signal(barrier, inc=1, device_id=(before // 2, (before % 2) * 2 + 1), device_id_type=MESH)

    mine = pl.ds(pl.multiple_of(EDGE + core * part, 16), part)
    load_hid = [pltpu.make_async_copy(hid.at[s], rows.at[s, mine, :], hid_local.at[s]) for s in range(seqs)]
    load_small = [
        pltpu.make_async_copy(src, dst, small_local.at[n])
        for n, (src, dst) in enumerate(
            [
                (wstep, wst), (cv, ctap.at[y, 0]), (ck, ctap.at[y, 1]), (newq, qraw.at[y]),
                (jump.at[:, :, pl.ds(pl.multiple_of(y * local, 128), local)], jall.at[y]),
                (newv, nraw.at[0]), (newk, nraw.at[1]), (newg, nraw.at[2]),
            ]
        )
    ]
    load_w = [
        pltpu.make_async_copy(w.at[:, pl.ds(a * 128, 128)], w_all.at[y, a, half], w_local.at[a, half])
        for a in range(groups)
        for half, w in enumerate((wv, wk))
    ]
    for c in load_hid + load_small + load_w:
        c.start()

    sub = lax.broadcasted_iota(jnp.int32, (heads, 128), 0)
    lane = lax.broadcasted_iota(jnp.int32, (heads, 128), 1)

    def by_head(ref):
        out = jnp.zeros((heads, 128), f32)
        for h in range(heads):
            out = jnp.where(sub == h, ref[h], out)
        return out

    def by_line(value_of):
        out = jnp.zeros((lines, 128), f32)
        for a in range(groups):
            for s in range(seqs):
                pair = jnp.where(lane < 64, value_of(s, 2 * a), value_of(s, 2 * a + 1))
                out = jnp.where(sub == a * seqs + s, pair, out)
        return out

    def lines_of(x):
        x = x.astype(f32)
        return jnp.concatenate([x[:, a * 128 : (a + 1) * 128] for a in range(groups)], axis=0)

    ball[y] = jnp.where(lane == 0, by_head(bias), jnp.where(lane == 1, by_head(rate), 0.0))
    new_size = softplus(by_line(lambda s, h: newstep[s, h]) + by_line(lambda s, h: bias[h]))
    keep = jnp.exp(-by_line(lambda s, h: rate[h]) * new_size)
    pl.semaphore_wait(barrier, chips + core)

    theirs = pl.ds(pl.multiple_of(far * local, 128), local)
    send_hid = [
        send(hid.at[s], rows.at[s, mine, :], hid_send.at[s], hid_recv.at[s], core_peer) for s in range(seqs)
    ]
    send_small = [
        send(src, dst, small_send.at[n], small_recv.at[n], y_peer)
        for n, (src, dst) in enumerate(
            [
                (jump.at[:, :, theirs], jall.at[y]), (ball.at[y], ball.at[y]),
                (cv, ctap.at[y, 0]), (ck, ctap.at[y, 1]), (newq, qraw.at[y]),
            ]
        )
    ]
    edge = [
        send(
            hid.at[:, pl.ds(part - TIP, TIP), :], rows.at[:, pl.ds(EDGE - TIP, TIP), :], edge_send.at[c], edge_recv,
            (after // 2, (after % 2) * 2 + c),
        )
        for c in range(2)
    ]
    count = 2 * PIECES
    diag = groups - 1 - quarter
    first, second = (3 * count) // 8, (6 * count) // 8

    def y_copy(half, n, a, chunk, rel):
        at = pl.ds(pl.multiple_of((chunk // 2) * depth, depth), depth)
        return send(
            (wv, wk)[half].at[at, pl.ds(pl.multiple_of(a * 128, 128), 128)],
            w_all.at[y, a, half, at, :], y_send.at[n], w_recv.at[rel, chunk], y_peer,
        )

    def start_y(n):
        if isinstance(n, int):
            a, chunk, rel = (quarter, n, 0) if n < count else (diag, second + n - count, 3)
            y_copy(chunk % 2, n, a, chunk, rel).start()
        else:
            for half in range(2):

                @pl.when(n % 2 == half)
                def _():
                    y_copy(half, n, quarter, n, 0).start()

    def w_copy(a, chunk, send_sem, rel, peer):
        block = w_all.at[
            far, a, chunk % 2, pl.ds(pl.multiple_of((chunk // 2) * depth, depth), depth), :
        ]
        return send(block, block, send_sem, w_recv.at[rel, chunk], peer)

    def wait_chunk(rel, a, chunk):
        w_copy(a, chunk, y_send.at[0], rel, y_peer).wait_recv()

    def relay(chunk):
        wait_chunk(0, quarter, chunk)
        w_copy(quarter, chunk, x_send.at[chunk], 1, x_peer).start()
        w_copy(quarter, chunk, z_send.at[chunk], 2, z_peer).start()

    qx, qz = flip(quarter, 1), flip(quarter, 2)

    def relay_diag(n):
        wait_chunk(1, qx, n)
        w_copy(qx, n, z_send.at[count + n], 3, z_peer).start()
        wait_chunk(2, qz, first + n)
        w_copy(qz, first + n, x_send.at[count + n], 3, x_peer).start()

    start_y(0)
    for c in send_hid + send_small:
        c.start()

    @pl.when(core == 1)
    def _():
        for c in edge:
            c.start()

    start_y(1)
    for c in load_small:
        c.wait()
    query = lines_of(qraw[y])
    gate = lines_of(nraw[2])
    gate = gate / (1.0 + jnp.exp(-gate))
    match = jnp.sum(lines_of(nraw[1]) * query, axis=1, keepdims=True)
    coef[0] = keep * gate
    coef[1] = new_size * lines_of(nraw[0]) * match * gate

    for c in load_hid:
        c.wait()
    for c in send_hid:
        c.wait_recv()
    relay(0)
    start_y(2)
    for s in range(seqs):
        step_t[s] = (
            lax.dot_general(wst[...], rows[s, EDGE:, :], (((1,), (1,)), ((), ())), preferred_element_type=f32)
            .astype(bf16)
            .astype(f32)
        )
    for c in send_small:
        c.wait_recv()
    for b in range(2):
        for half in range(2):
            ct = ctap[b, half].astype(f32) * 0.5
            for a in range(groups):
                tall[b, a, 0 : ct.shape[0], half * 128 : (half + 1) * 128] = ct[:, a * 128 : (a + 1) * 128]
        qall[b] = lines_of(qraw[b])
    relay(1)
    start_y(3)
    decays, sizes = [], []
    for yb in range(2):
        for s in range(seqs):
            raw = step_t[s, pl.ds(pl.multiple_of((2 * yb + core) * heads, 8), heads), :]
            one = softplus(raw + ball[yb, :, 0:1])
            sizes.append(one)
            decays.append(jall[yb, s] - ball[yb, :, 1:2] * one)
    size = jnp.concatenate(sizes, axis=0)
    decay = jnp.concatenate(decays, axis=0)
    packed = jnp.zeros((heads, 128), f32)
    for n, one in enumerate(decays):
        packed = jnp.where(lane == n * heads + sub, jnp.sum(one, axis=1, keepdims=True), packed)
    totals[0] = jnp.sum(packed, axis=0, keepdims=True)
    spot = lax.broadcasted_iota(jnp.int32, decay.shape, 1)
    suffix = jnp.where(spot < local - 1, pltpu.roll(decay, local - 1, 1), 0.0)
    shift = 1
    while shift < local:
        suffix = suffix + jnp.where(spot < local - shift, pltpu.roll(suffix, local - shift, 1), 0.0)
        shift *= 2
    weight = size * jnp.exp(suffix)
    for yb in range(2):
        for s in range(seqs):
            at = (yb * seqs + s) * heads
            wrow[yb, s] = weight[at : at + heads]
    send_tot = [
        send(totals.at[0], totals.at[r], tot_send.at[r], tot_recv.at[r], chip_peer(r)) for r in range(1, chips)
    ]
    for c in send_tot:
        c.start()
    relay(2)
    start_y(4)
    edge[0].wait_recv()

    @pl.when(order == 0)
    def _():
        rows[:, 0:EDGE, :] = jnp.zeros((seqs, EDGE, width), rows.dtype)

    for c in load_w:
        c.wait()

    def project(block, a, s):
        both = jnp.dot(
            rows[s], jnp.concatenate([w_all[block, a, 0], w_all[block, a, 1]], axis=1), preferred_element_type=f32
        )
        proj[2 * s] = both[:, :128]
        proj[2 * s + 1] = both[:, 128:]

    def mixed(slab, tap):
        half = proj[slab, EDGE - 3 : EDGE - 3 + local, :] * tap[0:1]
        for k in range(1, 4):
            half = half + proj[slab, EDGE - 3 + k : EDGE - 3 + k + local, :] * tap[k : k + 1]
        return half + half * jnp.tanh(half)

    def reduce_rows(slot, block, a, s):
        tap = tall[block, a]
        key = mixed(2 * s + 1, tap[:, 128:]).astype(bf16)
        val_t = mixed(2 * s, tap[:, :128]).astype(bf16).T.astype(f32)
        spread = jnp.concatenate(
            [jnp.broadcast_to(wrow[block, s, pl.ds(2 * a + p, 1), :], (64, local)) for p in range(2)], axis=0
        )
        sfull[slot, a, s] = jnp.dot((val_t * spread).astype(bf16), key, preferred_element_type=f32)

    def group(slot, block, a):
        project(block, a, 0)
        project(block, a, 1)
        reduce_rows(slot, block, a, 0)
        reduce_rows(slot, block, a, 1)

    def flush(slot, block, a, peers):
        for s in range(seqs):
            scale = jnp.concatenate(
                [jnp.broadcast_to(fac[block, s, pl.ds(2 * a + p, 1), :], (64, 128)) for p in range(2)], axis=0
            )
            state = sfull[slot, a, s] * scale
            parts = jnp.swapaxes(state.reshape(2, sp_count, share, 128), 0, 1).reshape(sp_count, per_share, 128)
            here = pl.ds(s * per_share, per_share)
            stage[slot, a, :, here, :] = parts.astype(bf16)
            if slot == 0:
                full[a, :, here, :] = parts
            line = a * seqs + s
            q = jnp.broadcast_to(qall[block, pl.ds(line, 1), :], (16, 128)).astype(bf16)
            high = state.astype(bf16)
            low = (state - high.astype(f32)).astype(bf16)
            dims = (((1,), (1,)), ((), ()))
            read = lax.dot_general(q, high, dims, preferred_element_type=f32) + lax.dot_general(
                q, low, dims, preferred_element_type=f32
            )
            reads[slot, pl.ds(line, 1), :] = read[0:1]
        for r in peers:
            send(
                stage.at[slot, a, xor_sp(r % sp_count)], got.at[r - 1, a], st_send, st_recv, chip_peer(r)
            ).start()

    def own_block(a, carry):
        relay(3 + a)

        @pl.when(a < groups - 1)
        def _():
            start_y(5 + a)

        @pl.when(a == groups - 1)
        def _():
            start_y(count)

        @pl.when(a >= 2)
        def _():
            relay_diag(a - 2)

        group(0, y, a)
        return carry

    lax.fori_loop(0, groups, own_block, 0)
    relay(count - 1)
    start_y(count + 1)
    relay_diag(2)

    later = jnp.zeros((1, 128), f32)
    for r in range(1, chips):
        send_tot[r - 1].wait_recv()
        source = xor_sp(r % sp_count) * 2 + (far if r >= sp_count else y)
        later = later + totals[r] * jnp.where(source > order, 1.0, 0.0)
    later = jnp.broadcast_to(later, (heads, 128))
    for yb in range(2):
        for s in range(seqs):
            n = yb * seqs + s
            one = jnp.sum(jnp.where(lane == n * heads + sub, later, 0.0), axis=1, keepdims=True)
            fac[yb, s] = jnp.broadcast_to(jnp.exp(one), (heads, 128))

    def send_reads(slot, r):
        return send(reads.at[slot], read_got.at[r], rd_send.at[r], rd_recv.at[r], chip_peer(r))

    waits = {
        1: list(range(first, count)),
        2: list(range(first)) + list(range(second, count)),
        3: list(range(count)),
    }

    def far_block(k, carry):
        a = (quarter % 2 + k % 2) % 2 + 2 * ((quarter // 2 + k // 2) % 2)
        for rel, chunks in waits.items():

            @pl.when(k == rel)
            def _():
                for chunk in chunks:
                    wait_chunk(rel, a, chunk)

        @pl.when(k == groups - 1)
        def _():
            for r in range(1, sp_count):
                send_reads(0, r).start()

        group(1, far, a)
        flush(1, far, a, range(sp_count, chips))

        @pl.when(k < groups - 1)
        def _():
            flush(0, y, k, range(1, sp_count))

        @pl.when(k == groups - 2)
        def _():
            flush(0, y, groups - 1, range(1, sp_count))

        return carry

    lax.fori_loop(0, groups, far_block, 0)

    send_rd = [send_reads(r // sp_count, r) for r in range(1, chips)]
    for c in send_rd[sp_count - 1 :]:
        c.start()
    everything = send(got, got, st_send, st_recv, y_peer)
    everything.wait_recv()
    for a in range(groups):
        final = full[a, sp]
        for r in range(chips - 1):
            final = final + got[r, a].astype(f32)
        for s in range(seqs):
            for p in range(2):
                at = s * per_share + p * share
                state_out[s, 2 * a + p] = final[at : at + share].astype(bf16)
    read = reads[0]
    for r in range(1, chips):
        send_rd[r - 1].wait_recv()
        read = read + read_got[r]
    gated = coef[0] * read + coef[1]
    mean = jnp.mean(gated * gated, axis=1, keepdims=True)
    read_out[...] = gated * lax.rsqrt(mean + EPSILON)

    @pl.when(core == 1)
    def _():
        for c in edge:
            c.wait_send()

    for c in send_hid + send_small + send_tot + send_rd + [everything]:
        c.wait_send()
    for n in range(count):
        y_copy(n % 2, n, quarter, n, 0).wait_send()
        w_copy(quarter, n, x_send.at[n], 1, x_peer).wait_send()
        w_copy(quarter, n, z_send.at[n], 2, z_peer).wait_send()
    for n in range(count - second):
        y_copy((second + n) % 2, count + n, diag, second + n, 3).wait_send()
    for n in range(first):
        w_copy(qx, n, z_send.at[count + n], 3, z_peer).wait_send()
        w_copy(qz, n, x_send.at[count + n], 3, x_peer).wait_send()


def per_device(
    hidden_in, w_value, w_key, w_step, conv_value, conv_key, step_bias, decay_rate, decay_jump,
    new_value, new_key, new_query, new_gate, new_step, read_gain,
):
    sp_count, tp_count = lax.axis_size("sp"), lax.axis_size("tp")
    heads = step_bias.shape[0]
    groups = w_key.shape[1] // STATE
    seqs, part, width = hidden_in.shape
    per = heads // groups
    share = HEAD_DIM // sp_count
    if not (tp_count == 4 and groups == 4 and share == 8 and per == 2 and seqs == 2 and part % 64 == 0):
        return general(
            hidden_in, w_value, w_key, w_step, conv_value, conv_key, step_bias, decay_rate, decay_jump,
            new_value, new_key, new_query, new_gate, new_step, read_gain,
        )
    f32, bf16 = jnp.float32, jnp.bfloat16
    sp_index = lax.axis_index("sp")
    local = 2 * part
    tap_count = conv_value.shape[0]
    chips = 2 * sp_count
    block = seqs * per * share
    lines = groups * seqs
    cols = w_value.shape[1]
    vmem, anyspace = pl.BlockSpec(memory_space=pltpu.VMEM), pl.BlockSpec(memory_space=pl.ANY)
    smem = pl.BlockSpec(memory_space=pltpu.SMEM)
    dma = pltpu.SemaphoreType.DMA
    count = 2 * PIECES
    state, read = pl.pallas_call(
        mixer_kernel,
        out_shape=(
            jax.ShapeDtypeStruct((seqs, heads, share, STATE), bf16),
            jax.ShapeDtypeStruct((lines, 128), f32),
        ),
        in_specs=[anyspace] * 11 + [smem] * 3,
        out_specs=(vmem, vmem),
        scratch_shapes=[
            pltpu.VMEM((seqs, EDGE + local, width), bf16),
            pltpu.VMEM((2, groups, 2, width, 128), bf16),
            pltpu.VMEM((w_step.shape[1], width), bf16),
            pltpu.VMEM((2, 2, tap_count, cols), bf16),
            pltpu.VMEM((2, groups, 8, 256), f32),
            pltpu.VMEM((2, seqs, heads, local), f32),
            pltpu.VMEM((2, heads, 128), f32),
            pltpu.VMEM((3, seqs, cols), bf16),
            pltpu.VMEM((2, seqs, cols), bf16),
            pltpu.VMEM((2, lines, 128), f32),
            pltpu.VMEM((2, lines, 128), f32),
            pltpu.VMEM((seqs, 4 * heads, local), f32),
            pltpu.VMEM((2, seqs, heads, local), f32),
            pltpu.VMEM((4, EDGE + local, 128), f32),
            pltpu.VMEM((2, groups, seqs, 128, 128), f32),
            pltpu.VMEM((2, seqs, heads, 128), f32),
            pltpu.VMEM((chips, 1, 128), f32),
            pltpu.VMEM((2, groups, sp_count, block, 128), bf16),
            pltpu.VMEM((groups, sp_count, block, 128), f32),
            pltpu.VMEM((chips - 1, groups, block, 128), bf16),
            pltpu.VMEM((2, lines, 128), f32),
            pltpu.VMEM((chips, lines, 128), f32),
            dma((seqs,)), dma((seqs,)), dma((seqs,)), dma((groups, 2)), dma((8,)), dma((2,)), dma, dma((5,)), dma((5,)),
            dma((2 * count,)), dma((2 * count,)), dma((2 * count,)), dma((4, count)),
            dma((chips,)), dma((chips,)), dma, dma, dma((chips,)), dma((chips,)),
        ],
        compiler_params=pltpu.CompilerParams(
            collective_id=0, has_side_effects=True, vmem_limit_bytes=60 * 1024 * 1024
        ),
    )(
        hidden_in, w_value, w_key, jnp.swapaxes(w_step, 0, 1), conv_value, conv_key, jnp.swapaxes(decay_jump, 1, 2),
        new_value, new_key, new_query, new_gate, step_bias, decay_rate, new_step,
    )

    read = lax.dynamic_slice_in_dim(read.reshape(groups, seqs, per, HEAD_DIM), sp_index * share, share, 3)
    gain = lax.dynamic_slice_in_dim(read_gain.reshape(groups, 1, per, HEAD_DIM), sp_index * share, share, 3)
    read = jnp.swapaxes(read * gain.astype(f32), 0, 1)
    return state, read.reshape(seqs, heads, share).astype(bf16)


def solution(mesh):
    return jax.shard_map(
        per_device,
        mesh=mesh,
        in_specs=(
            P(None, ("sp", "tp"), None),
            P(None, "tp"),
            P(None, "tp"),
            P(),
            P(None, "tp"),
            P(None, "tp"),
            P("tp"),
            P("tp"),
            P(None, "sp", "tp"),
            P(None, "tp"),
            P(None, "tp"),
            P(None, "tp"),
            P(None, "tp"),
            P(None, "tp"),
            P("tp"),
        ),
        out_specs=(P(None, "tp", "sp", None), P(None, "tp", "sp")),
        check_vma=False,
    )
```

```python
import jax
import jax.numpy as jnp
from jax import lax
from jax.experimental import pallas as pl
from jax.experimental.pallas import tpu as pltpu
from jax.sharding import PartitionSpec as P

HEAD_DIM = 64
STATE = 128


EPSILON = 1e-05


def shifted(value, axis, steps):
    count = lax.axis_size(axis)
    leading, last = (max(0, -steps), min(count, count - steps))
    return lax.ppermute(value, axis, [(source, source + steps) for source in range(leading, last)])


def causal_mix(padded_rows, conv_taps):
    tap_count = conv_taps.shape[0]
    length = padded_rows.shape[-2] - tap_count + 1
    running = jnp.zeros(padded_rows.shape[:-2] + (length, padded_rows.shape[-1]), jnp.float32)
    for tap_index in range(tap_count):
        running = running + padded_rows[..., tap_index : tap_index + length, :].astype(
            jnp.float32
        ) * conv_taps[tap_index].astype(jnp.float32)
    return running


def block_states(mixed_rows, weight, value_cols, groups_dev):
    seq_count, row_count, heads_dev = weight.shape
    per_group = heads_dev // groups_dev
    values = (
        mixed_rows[:, :, :value_cols].reshape(seq_count, row_count, groups_dev, per_group, HEAD_DIM)
        * weight.reshape(seq_count, row_count, groups_dev, per_group)[..., None]
    )
    keys = mixed_rows[:, :, value_cols:].reshape(seq_count, row_count, groups_dev, STATE)
    states = jnp.einsum("slgep,slgn->sgepn", values, keys, precision=lax.Precision.HIGHEST)
    return states.reshape(seq_count, heads_dev, HEAD_DIM, STATE)


def general(
    hidden_in,
    w_value,
    w_key,
    w_step,
    conv_value,
    conv_key,
    step_bias,
    decay_rate,
    decay_jump,
    new_value,
    new_key,
    new_query,
    new_gate,
    new_step,
    read_gain,
):
    sp_count = lax.axis_size("sp")
    sp_index = lax.axis_index("sp")
    tp_index = lax.axis_index("tp")
    heads_dev = step_bias.shape[0]
    value_cols = w_value.shape[1]
    key_cols = w_key.shape[1]
    groups_dev = key_cols // STATE
    per_group = heads_dev // groups_dev
    kernel_taps = conv_value.shape[0]
    seq_count = hidden_in.shape[0]
    share = HEAD_DIM // sp_count
    own_step = lax.dynamic_slice_in_dim(w_step, tp_index * heads_dev, heads_dev, 1)
    w_joined = jnp.concatenate([w_value, w_key, own_step], axis=1)
    projected = jnp.einsum(
        "tfy,yz->tfz",
        lax.all_gather(hidden_in, "tp", axis=1, tiled=True),
        w_joined,
        preferred_element_type=jnp.float32,
    ).astype(jnp.bfloat16)
    seg_rows = projected.shape[1]
    proj_pair = projected[:, :, : value_cols + key_cols]
    proj_step = projected[:, :, value_cols + key_cols :]
    step_size = jax.nn.softplus(proj_step.astype(jnp.float32) + step_bias)
    log_decay = decay_jump - decay_rate * step_size
    conv_taps = jnp.concatenate([conv_value, conv_key], axis=1)
    edge_rows = shifted(proj_pair[:, seg_rows - (kernel_taps - 1) :, :], "sp", 1)
    mixed_rows = jax.nn.silu(causal_mix(jnp.concatenate([edge_rows, proj_pair], axis=1), conv_taps))
    seg_total = jnp.sum(log_decay, axis=1)
    decay_after = seg_total[:, None, :] - jnp.cumsum(log_decay, axis=1)
    seg_states = block_states(mixed_rows, step_size * jnp.exp(decay_after), value_cols, groups_dev)
    tiled_totals = jnp.broadcast_to(
        seg_total[:, None, :, None], (seq_count, 1, heads_dev, sp_count)
    )
    got_states, got_totals = (
        lax.all_to_all(seg_states[:, None], "sp", split_axis=3, concat_axis=1, tiled=True),
        lax.all_to_all(tiled_totals, "sp", split_axis=3, concat_axis=1, tiled=True),
    )
    got_totals = got_totals[..., 0]
    tail_decay = jnp.sum(got_totals, axis=1, keepdims=True) - jnp.cumsum(got_totals, axis=1)
    final_state = jnp.einsum(
        "sjh,sjhpn->shpn", jnp.exp(tail_decay), got_states, precision=lax.Precision.HIGHEST
    )
    cache_state = final_state.astype(jnp.bfloat16)
    new_size = jax.nn.softplus(new_step + step_bias)
    keep_share = jnp.exp(-decay_rate * new_size)
    query = new_query.astype(jnp.float32).reshape(seq_count, groups_dev, STATE)
    own_key = new_key.astype(jnp.float32).reshape(seq_count, groups_dev, STATE)
    key_match = jnp.sum(own_key * query, axis=-1)
    size_grid = new_size.reshape(seq_count, groups_dev, per_group)
    keep_grid = keep_share.reshape(seq_count, groups_dev, per_group)
    value_grid = new_value.astype(jnp.float32).reshape(seq_count, groups_dev, per_group, HEAD_DIM)
    gate_grid = jax.nn.silu(new_gate.astype(jnp.float32)).reshape(
        seq_count, groups_dev, per_group, HEAD_DIM
    )
    gain_grid = read_gain.astype(jnp.float32).reshape(groups_dev, per_group, HEAD_DIM)
    own_value = lax.dynamic_slice_in_dim(value_grid, sp_index * share, share, 3)
    own_gate = lax.dynamic_slice_in_dim(gate_grid, sp_index * share, share, 3)
    own_gain = lax.dynamic_slice_in_dim(gain_grid, sp_index * share, share, 2)
    state_read = jnp.einsum(
        "sgepn,sgn->sgep",
        final_state.reshape(seq_count, groups_dev, per_group, share, STATE),
        query,
        precision=lax.Precision.HIGHEST,
    )
    raw_read = (
        keep_grid[..., None] * state_read
        + size_grid[..., None] * own_value * key_match[:, :, None, None]
    )
    gated = raw_read * own_gate
    squares = lax.psum(jnp.sum(gated * gated, axis=(2, 3)), "sp")
    scale = lax.rsqrt(squares / (per_group * HEAD_DIM) + EPSILON)
    read_out = (gated * scale[:, :, None, None] * own_gain).astype(jnp.bfloat16)
    return (cache_state, read_out.reshape(seq_count, heads_dev, share))


MESH = pl.DeviceIdType.MESH
PIECES = 8
Y_AHEAD = 4
EDGE = 16
TIP = 8


def softplus(x):
    return jnp.maximum(x, 0.0) + jnp.log1p(jnp.exp(-jnp.abs(x)))


def flip(value, bit):
    return value + bit - 2 * bit * ((value // bit) % 2)


def mixer_kernel(
    hid, wv, wk, wstep, cv, ck, jump, newv, newk, newq, newg, gain, bias, rate, newstep,
    state_out, read_out,
    rows, w_all, wst, gvec, ctap, tall, jall, ball, nraw, qraw, qall, coef, step_t, wrow, proj, sfull, fac, totals,
    stage, full, got, reads, read_got,
    hid_local, hid_send, hid_recv, w_local, small_local, edge_send, edge_recv, small_send, small_recv,
    y_send, x_send, z_send, w_recv, tot_send, tot_recv, st_send, st_recv, rd_send, rd_recv,
):
    sp, tp = lax.axis_index("sp"), lax.axis_index("tp")
    sp_count = lax.axis_size("sp")
    y, core = tp // 2, tp % 2
    far = 1 - y
    chips = 2 * sp_count
    seqs, part, width = hid.shape
    local = 2 * part
    depth = width // PIECES
    groups = w_all.shape[1]
    heads = jump.shape[1]
    lines = groups * seqs
    share = 64 // sp_count
    per_share = stage.shape[3] // seqs
    quarter = sp % 4
    f32, bf16 = jnp.float32, jnp.bfloat16

    def xor_sp(bits):
        out, bit = sp, 1
        while bit < sp_count:
            if bits & bit:
                out = flip(out, bit)
            bit *= 2
        return out

    x_peer, z_peer, y_peer = (flip(sp, 1), tp), (flip(sp, 2), tp), (sp, flip(tp, 2))
    core_peer = (sp, flip(tp, 1))

    def chip_peer(r):
        return (xor_sp(r % sp_count), flip(tp, 2) if r >= sp_count else tp)

    def send(src, dst, send_sem, recv_sem, peer):
        return pltpu.make_async_remote_copy(
            src_ref=src, dst_ref=dst, send_sem=send_sem, recv_sem=recv_sem, device_id=peer, device_id_type=MESH
        )

    order = sp * 2 + y
    after = lax.rem(order + 1, chips)
    before = lax.rem(order + chips - 1, chips)

    barrier = pltpu.get_barrier_semaphore()
    for r in range(1, chips):
        pl.semaphore_signal(barrier, inc=1, device_id=chip_peer(r), device_id_type=MESH)
    pl.semaphore_signal(barrier, inc=1, device_id=core_peer, device_id_type=MESH)

    @pl.when(core == 0)
    def _():
        pl.semaphore_signal(barrier, inc=1, device_id=(before // 2, (before % 2) * 2 + 1), device_id_type=MESH)

    mine = pl.ds(pl.multiple_of(EDGE + core * part, 16), part)
    load_hid = [pltpu.make_async_copy(hid.at[s], rows.at[s, mine, :], hid_local.at[s]) for s in range(seqs)]
    load_small = [
        pltpu.make_async_copy(src, dst, small_local.at[n])
        for n, (src, dst) in enumerate(
            [
                (wstep, wst), (cv, ctap.at[y, 0]), (ck, ctap.at[y, 1]), (newq, qraw.at[y]),
                (jump.at[:, :, pl.ds(pl.multiple_of(y * local, 128), local)], jall.at[y]),
                (newv, nraw.at[0]), (newk, nraw.at[1]), (newg, nraw.at[2]), (gain, gvec),
            ]
        )
    ]
    load_w = [
        pltpu.make_async_copy(w.at[:, pl.ds(a * 128, 128)], w_all.at[y, a, half], w_local.at[a, half])
        for a in range(groups)
        for half, w in enumerate((wv, wk))
    ]
    for c in load_hid + load_small + load_w:
        c.start()

    sub = lax.broadcasted_iota(jnp.int32, (heads, 128), 0)
    lane = lax.broadcasted_iota(jnp.int32, (heads, 128), 1)

    def by_head(ref):
        out = jnp.zeros((heads, 128), f32)
        for h in range(heads):
            out = jnp.where(sub == h, ref[h], out)
        return out

    def by_line(value_of):
        out = jnp.zeros((lines, 128), f32)
        for a in range(groups):
            for s in range(seqs):
                pair = jnp.where(lane < 64, value_of(s, 2 * a), value_of(s, 2 * a + 1))
                out = jnp.where(sub == a * seqs + s, pair, out)
        return out

    def lines_of(x):
        x = x.astype(f32)
        return jnp.concatenate([x[:, a * 128 : (a + 1) * 128] for a in range(groups)], axis=0)

    ball[y] = jnp.where(lane == 0, by_head(bias), jnp.where(lane == 1, by_head(rate), 0.0))
    new_size = softplus(by_line(lambda s, h: newstep[s, h]) + by_line(lambda s, h: bias[h]))
    keep = jnp.exp(-by_line(lambda s, h: rate[h]) * new_size)
    pl.semaphore_wait(barrier, chips + core)

    theirs = pl.ds(pl.multiple_of(far * local, 128), local)
    send_hid = [
        send(hid.at[s], rows.at[s, mine, :], hid_send.at[s], hid_recv.at[s], core_peer) for s in range(seqs)
    ]
    send_small = [
        send(src, dst, small_send.at[n], small_recv.at[n], y_peer)
        for n, (src, dst) in enumerate(
            [
                (jump.at[:, :, theirs], jall.at[y]), (ball.at[y], ball.at[y]),
                (cv, ctap.at[y, 0]), (ck, ctap.at[y, 1]), (newq, qraw.at[y]),
            ]
        )
    ]
    edge = [
        send(
            hid.at[:, pl.ds(part - TIP, TIP), :], rows.at[:, pl.ds(EDGE - TIP, TIP), :], edge_send.at[c], edge_recv,
            (after // 2, (after % 2) * 2 + c),
        )
        for c in range(2)
    ]
    count = 2 * PIECES
    diag = groups - 1 - quarter
    z_part, second = count // 4, count // 4 + (5 * count) // 16
    x_part, y_part = second - z_part, count - second

    def y_copy(half, n, a, chunk, rel):
        at = pl.ds(pl.multiple_of((chunk // 2) * depth, depth), depth)
        return send(
            (wv, wk)[half].at[at, pl.ds(pl.multiple_of(a * 128, 128), 128)],
            w_all.at[y, a, half, at, :], y_send.at[n], w_recv.at[rel, chunk], y_peer,
        )

    def start_y(n):
        for half in range(2):

            @pl.when(jnp.logical_and(n < count, n % 2 == half))
            def _():
                y_copy(half, n, quarter, n, 0).start()

            @pl.when(jnp.logical_and(n >= count, (n - count + second) % 2 == half))
            def _():
                y_copy(half, n, diag, n - count + second, 3).start()

    def w_copy(a, chunk, send_sem, rel, peer):
        block = w_all.at[
            far, a, chunk % 2, pl.ds(pl.multiple_of((chunk // 2) * depth, depth), depth), :
        ]
        return send(block, block, send_sem, w_recv.at[rel, chunk], peer)

    def wait_chunk(rel, a, chunk):
        w_copy(a, chunk, y_send.at[0], rel, y_peer).wait_recv()

    def relay(chunk):
        wait_chunk(0, quarter, chunk)
        w_copy(quarter, chunk, x_send.at[chunk], 1, x_peer).start()
        w_copy(quarter, chunk, z_send.at[chunk], 2, z_peer).start()

        @pl.when(chunk + Y_AHEAD < count + y_part)
        def _():
            start_y(chunk + Y_AHEAD)

    qx, qz = flip(quarter, 1), flip(quarter, 2)

    def relay_diag(n):
        if n < z_part:
            wait_chunk(1, qx, n)
            w_copy(qx, n, z_send.at[count + n], 3, z_peer).start()
        if n < x_part:
            wait_chunk(2, qz, z_part + n)
            w_copy(qz, z_part + n, x_send.at[count + n], 3, x_peer).start()

    start_y(0)
    start_y(1)
    for c in send_hid + send_small:
        c.start()

    @pl.when(core == 1)
    def _():
        for c in edge:
            c.start()

    for n in range(2, Y_AHEAD):
        start_y(n)
    for c in load_small:
        c.wait()
    query = lines_of(qraw[y])
    gate = lines_of(nraw[2])
    gate = gate / (1.0 + jnp.exp(-gate))
    match = jnp.sum(lines_of(nraw[1]) * query, axis=1, keepdims=True)
    coef[0] = keep * gate
    coef[1] = new_size * lines_of(nraw[0]) * match * gate
    gains = jnp.zeros((lines, 128), f32)
    for a in range(groups):
        one = gvec[a * 128 : (a + 1) * 128].astype(f32).reshape(1, 128)
        gains = jnp.where(sub // seqs == a, jnp.broadcast_to(one, (lines, 128)), gains)
    coef[2] = gains

    relay(0)
    for c in load_hid:
        c.wait()
    for c in send_hid:
        c.wait_recv()
    relay(1)
    for s in range(seqs):
        step_t[s] = (
            lax.dot_general(wst[...], rows[s, EDGE:, :], (((1,), (1,)), ((), ())), preferred_element_type=f32)
            .astype(bf16)
            .astype(f32)
        )
    for c in send_small:
        c.wait_recv()
    for b in range(2):
        for half in range(2):
            ct = ctap[b, half].astype(f32) * 0.5
            for a in range(groups):
                tall[b, a, 0 : ct.shape[0], half * 128 : (half + 1) * 128] = ct[:, a * 128 : (a + 1) * 128]
        qall[b] = lines_of(qraw[b])
    relay(2)
    decays, sizes = [], []
    for yb in range(2):
        for s in range(seqs):
            raw = step_t[s, pl.ds(pl.multiple_of((2 * yb + core) * heads, 8), heads), :]
            one = softplus(raw + ball[yb, :, 0:1])
            sizes.append(one)
            decays.append(jall[yb, s] - ball[yb, :, 1:2] * one)
    size = jnp.concatenate(sizes, axis=0)
    decay = jnp.concatenate(decays, axis=0)
    packed = jnp.zeros((heads, 128), f32)
    for n, one in enumerate(decays):
        packed = jnp.where(lane == n * heads + sub, jnp.sum(one, axis=1, keepdims=True), packed)
    totals[0] = jnp.sum(packed, axis=0, keepdims=True)
    spot = lax.broadcasted_iota(jnp.int32, decay.shape, 1)
    suffix = jnp.where(spot < local - 1, pltpu.roll(decay, local - 1, 1), 0.0)
    shift = 1
    while shift < local:
        suffix = suffix + jnp.where(spot < local - shift, pltpu.roll(suffix, local - shift, 1), 0.0)
        shift *= 2
    weight = size * jnp.exp(suffix)
    for yb in range(2):
        for s in range(seqs):
            at = (yb * seqs + s) * heads
            wrow[yb, s] = weight[at : at + heads]
    send_tot = [
        send(totals.at[0], totals.at[r], tot_send.at[r], tot_recv.at[r], chip_peer(r)) for r in range(1, chips)
    ]
    for c in send_tot:
        c.start()
    relay(3)
    edge[0].wait_recv()

    @pl.when(order == 0)
    def _():
        rows[:, 0:EDGE, :] = jnp.zeros((seqs, EDGE, width), rows.dtype)

    for c in load_w:
        c.wait()

    def project(block, a, s):
        both = jnp.dot(
            rows[s], jnp.concatenate([w_all[block, a, 0], w_all[block, a, 1]], axis=1), preferred_element_type=f32
        )
        proj[2 * s] = both[:, :128]
        proj[2 * s + 1] = both[:, 128:]

    def mixed(slab, tap):
        half = proj[slab, EDGE - 3 : EDGE - 3 + local, :] * tap[0:1]
        for k in range(1, 4):
            half = half + proj[slab, EDGE - 3 + k : EDGE - 3 + k + local, :] * tap[k : k + 1]
        return half + half * jnp.tanh(half)

    def reduce_rows(slot, block, a, s):
        tap = tall[block, a]
        key = mixed(2 * s + 1, tap[:, 128:]).astype(bf16)
        val_t = mixed(2 * s, tap[:, :128]).astype(bf16).T.astype(f32)
        spread = jnp.concatenate(
            [jnp.broadcast_to(wrow[block, s, pl.ds(2 * a + p, 1), :], (64, local)) for p in range(2)], axis=0
        )
        sfull[slot, a, s] = jnp.dot((val_t * spread).astype(bf16), key, preferred_element_type=f32)

    def group(slot, block, a):
        project(block, a, 0)
        project(block, a, 1)
        reduce_rows(slot, block, a, 0)
        reduce_rows(slot, block, a, 1)

    def flush(slot, block, a, peers):
        for s in range(seqs):
            scale = jnp.concatenate(
                [jnp.broadcast_to(fac[block, s, pl.ds(2 * a + p, 1), :], (64, 128)) for p in range(2)], axis=0
            )
            state = sfull[slot, a, s] * scale
            parts = jnp.swapaxes(state.reshape(2, sp_count, share, 128), 0, 1).reshape(sp_count, per_share, 128)
            here = pl.ds(s * per_share, per_share)
            stage[slot, a, :, here, :] = parts.astype(bf16)
            if slot == 0:
                full[a, :, here, :] = parts
            line = a * seqs + s
            q = jnp.broadcast_to(qall[block, pl.ds(line, 1), :], (16, 128)).astype(bf16)
            high = state.astype(bf16)
            low = (state - high.astype(f32)).astype(bf16)
            dims = (((1,), (1,)), ((), ()))
            read = lax.dot_general(q, high, dims, preferred_element_type=f32) + lax.dot_general(
                q, low, dims, preferred_element_type=f32
            )
            reads[slot, pl.ds(line, 1), :] = read[0:1]
        for r in peers:
            send(
                stage.at[slot, a, xor_sp(r % sp_count)], got.at[r - 1, a], st_send, st_recv, chip_peer(r)
            ).start()

    def own_block(a, carry):
        relay(4 + 2 * a)
        relay(5 + 2 * a)
        group(0, y, a)
        return carry

    lax.fori_loop(0, groups, own_block, 0)
    for n in range(4 + 2 * groups, count):
        relay(n)
    for n in range(count + Y_AHEAD, count + y_part):
        start_y(n)
    for n in range(max(z_part, x_part)):
        relay_diag(n)

    later = jnp.zeros((1, 128), f32)
    for r in range(1, chips):
        send_tot[r - 1].wait_recv()
        source = xor_sp(r % sp_count) * 2 + (far if r >= sp_count else y)
        later = later + totals[r] * jnp.where(source > order, 1.0, 0.0)
    later = jnp.broadcast_to(later, (heads, 128))
    for yb in range(2):
        for s in range(seqs):
            n = yb * seqs + s
            one = jnp.sum(jnp.where(lane == n * heads + sub, later, 0.0), axis=1, keepdims=True)
            fac[yb, s] = jnp.broadcast_to(jnp.exp(one), (heads, 128))

    def send_reads(slot, r):
        return send(reads.at[slot], read_got.at[r], rd_send.at[r], rd_recv.at[r], chip_peer(r))

    waits = {
        1: list(range(z_part, count)),
        2: list(range(z_part)) + list(range(second, count)),
        3: list(range(count)),
    }

    def far_block(k, carry):
        a = (quarter % 2 + k % 2) % 2 + 2 * ((quarter // 2 + k // 2) % 2)
        for rel, chunks in waits.items():

            @pl.when(k == rel)
            def _():
                for chunk in chunks:
                    wait_chunk(rel, a, chunk)

        @pl.when(k == groups - 1)
        def _():
            for r in range(1, sp_count):
                send_reads(0, r).start()

        group(1, far, a)
        flush(1, far, a, range(sp_count, chips))

        @pl.when(k < groups - 1)
        def _():
            flush(0, y, k, range(1, sp_count))

        @pl.when(k == groups - 2)
        def _():
            flush(0, y, groups - 1, range(1, sp_count))

        return carry

    lax.fori_loop(0, groups, far_block, 0)

    send_rd = [send_reads(r // sp_count, r) for r in range(1, chips)]
    for c in send_rd[sp_count - 1 :]:
        c.start()
    everything = send(got, got, st_send, st_recv, y_peer)
    everything.wait_recv()
    for a in range(groups):
        final = full[a, sp]
        for r in range(chips - 1):
            final = final + got[r, a].astype(f32)
        for s in range(seqs):
            for p in range(2):
                at = s * per_share + p * share
                state_out[s, 2 * a + p] = final[at : at + share].astype(bf16)
    read = reads[0]
    for r in range(1, chips):
        send_rd[r - 1].wait_recv()
        read = read + read_got[r]
    gated = coef[0] * read + coef[1]
    mean = jnp.mean(gated * gated, axis=1, keepdims=True)
    normed = gated * lax.rsqrt(mean + EPSILON) * coef[2]
    left = pltpu.roll(normed, 128 - sp * share, 1)
    right = pltpu.roll(left, 64, 1)
    even = sub % 2 == 0
    read_out[0] = jnp.where(even, left, pltpu.roll(right, 1, 0))[:, :share].astype(bf16)
    read_out[1] = jnp.where(even, pltpu.roll(left, lines - 1, 0), right)[:, :share].astype(bf16)

    @pl.when(core == 1)
    def _():
        for c in edge:
            c.wait_send()

    for c in send_hid + send_small + send_tot + send_rd + [everything]:
        c.wait_send()
    for n in range(count):
        y_copy(n % 2, n, quarter, n, 0).wait_send()
        w_copy(quarter, n, x_send.at[n], 1, x_peer).wait_send()
        w_copy(quarter, n, z_send.at[n], 2, z_peer).wait_send()
    for n in range(y_part):
        y_copy((second + n) % 2, count + n, diag, second + n, 3).wait_send()
    for n in range(z_part):
        w_copy(qx, n, z_send.at[count + n], 3, z_peer).wait_send()
    for n in range(x_part):
        w_copy(qz, z_part + n, x_send.at[count + n], 3, x_peer).wait_send()


def per_device(
    hidden_in, w_value, w_key, w_step, conv_value, conv_key, step_bias, decay_rate, decay_jump,
    new_value, new_key, new_query, new_gate, new_step, read_gain,
):
    sp_count, tp_count = lax.axis_size("sp"), lax.axis_size("tp")
    heads = step_bias.shape[0]
    groups = w_key.shape[1] // STATE
    seqs, part, width = hidden_in.shape
    per = heads // groups
    share = HEAD_DIM // sp_count
    if not (tp_count == 4 and groups == 4 and share == 8 and per == 2 and seqs == 2 and part % 64 == 0):
        return general(
            hidden_in, w_value, w_key, w_step, conv_value, conv_key, step_bias, decay_rate, decay_jump,
            new_value, new_key, new_query, new_gate, new_step, read_gain,
        )
    f32, bf16 = jnp.float32, jnp.bfloat16
    local = 2 * part
    tap_count = conv_value.shape[0]
    chips = 2 * sp_count
    block = seqs * per * share
    lines = groups * seqs
    cols = w_value.shape[1]
    vmem, anyspace = pl.BlockSpec(memory_space=pltpu.VMEM), pl.BlockSpec(memory_space=pl.ANY)
    smem = pl.BlockSpec(memory_space=pltpu.SMEM)
    dma = pltpu.SemaphoreType.DMA
    count = 2 * PIECES
    state, read = pl.pallas_call(
        mixer_kernel,
        out_shape=(
            jax.ShapeDtypeStruct((seqs, heads, share, STATE), bf16),
            jax.ShapeDtypeStruct((seqs, heads, share), bf16),
        ),
        in_specs=[anyspace] * 12 + [smem] * 3,
        out_specs=(vmem, vmem),
        scratch_shapes=[
            pltpu.VMEM((seqs, EDGE + local, width), bf16),
            pltpu.VMEM((2, groups, 2, width, 128), bf16),
            pltpu.VMEM((w_step.shape[1], width), bf16),
            pltpu.VMEM((cols,), bf16),
            pltpu.VMEM((2, 2, tap_count, cols), bf16),
            pltpu.VMEM((2, groups, 8, 256), f32),
            pltpu.VMEM((2, seqs, heads, local), f32),
            pltpu.VMEM((2, heads, 128), f32),
            pltpu.VMEM((3, seqs, cols), bf16),
            pltpu.VMEM((2, seqs, cols), bf16),
            pltpu.VMEM((2, lines, 128), f32),
            pltpu.VMEM((3, lines, 128), f32),
            pltpu.VMEM((seqs, 4 * heads, local), f32),
            pltpu.VMEM((2, seqs, heads, local), f32),
            pltpu.VMEM((4, EDGE + local, 128), f32),
            pltpu.VMEM((2, groups, seqs, 128, 128), f32),
            pltpu.VMEM((2, seqs, heads, 128), f32),
            pltpu.VMEM((chips, 1, 128), f32),
            pltpu.VMEM((2, groups, sp_count, block, 128), bf16),
            pltpu.VMEM((groups, sp_count, block, 128), f32),
            pltpu.VMEM((chips - 1, groups, block, 128), bf16),
            pltpu.VMEM((2, lines, 128), f32),
            pltpu.VMEM((chips, lines, 128), f32),
            dma((seqs,)), dma((seqs,)), dma((seqs,)), dma((groups, 2)), dma((9,)), dma((2,)), dma, dma((5,)), dma((5,)),
            dma((2 * count,)), dma((2 * count,)), dma((2 * count,)), dma((4, count)),
            dma((chips,)), dma((chips,)), dma, dma, dma((chips,)), dma((chips,)),
        ],
        compiler_params=pltpu.CompilerParams(
            collective_id=0, has_side_effects=True, vmem_limit_bytes=60 * 1024 * 1024
        ),
    )(
        hidden_in, w_value, w_key, jnp.swapaxes(w_step, 0, 1), conv_value, conv_key, jnp.swapaxes(decay_jump, 1, 2),
        new_value, new_key, new_query, new_gate, read_gain, step_bias, decay_rate, new_step,
    )

    return state, read


def solution(mesh):
    return jax.shard_map(
        per_device,
        mesh=mesh,
        in_specs=(
            P(None, ("sp", "tp"), None),
            P(None, "tp"),
            P(None, "tp"),
            P(),
            P(None, "tp"),
            P(None, "tp"),
            P("tp"),
            P("tp"),
            P(None, "sp", "tp"),
            P(None, "tp"),
            P(None, "tp"),
            P(None, "tp"),
            P(None, "tp"),
            P(None, "tp"),
            P("tp"),
        ),
        out_specs=(P(None, "tp", "sp", None), P(None, "tp", "sp")),
        check_vma=False,
    )
```
